512 devices in a mesh: fs: 64 (over z, y), tp: 8 (over x, core).
Axes of the slice: x: 4, y: 4, z: 16, core: 2. Of those that a mesh axis runs over, the one named last changes fastest.
Arguments:
- inputs: bfloat16 [16384, 2048], P('fs'), may hold values from -6 to 6
- query_cot: bfloat16 [16384, 1024], P('fs', 'tp'), may hold values from -0.046875 to 0.046875
- query_basis: bfloat16 [2048, 256], P('fs'), may hold values from -0.125 to 0.125
- query_master: float32 [2048, 1024], P('fs', 'tp'), may hold values from -3 to 3
- query_first: float32 [256, 1024], P('fs', 'tp'), may hold values from -4 to 4
- query_second: float32 [256, 1024], P('fs', 'tp'), may hold values from 0.02 to 4
Outputs:
- query_step: float32 [2048, 1024], P('fs', 'tp')
- query_first_new: float32 [256, 1024], P('fs', 'tp')
- query_second_new: float32 [256, 1024], P('fs', 'tp')
- query_copy: bfloat16 [2048, 1024], P('fs', 'tp')
The draws below stay inside these ranges and needn't reach their ends.
All inputs are finite; a program needn't handle non-finite values.
Results may differ from the reference program's by a relative error of at most 0.0011.
Values may be sent and summed in bfloat16 or wider, within the bound.
No kernel may reach another device: no remote copies, remote signals or barrier semaphores. Data moves between devices by JAX's collectives and lax.ppermute only.
A program may use at most 64 MiB of HBM per device.

```python
import math
import jax
import jax.numpy as jnp
from jax import lax

D = 2048
HEADS = 8
DQK = 128
RANK = 256
TOK_DEV = 256
TOKENS = 16384
NQ = 1024
N_FS = 64


def levels(key, extent, pieces, least, top_value):
    def one(position, blocks):
        heights = jax.random.uniform(jax.random.fold_in(jax.random.fold_in(key, 6), position), (blocks,), jnp.float32, least / len(pieces), top_value / len(pieces))
        return jnp.repeat(jnp.exp(heights), extent[position] // blocks).reshape((-1,) + (1,) * (len(extent) - position - 1))

    level = one(*pieces[0])
    for cut in pieces[1:]:
        level = level * one(*cut)
    return level


def scatter_about(rng, dims, spread, reach, pieces=(), dtype=jnp.bfloat16):
    values = jax.random.normal(rng, dims, jnp.float32) * spread
    if len(pieces) > 0:
        values = levels(rng, dims, pieces, -0.22, 0.18) * values
    return jnp.clip(values, min=-reach, max=reach).astype(dtype)


def setup_inputs(seed: int = 0) -> dict:
    streams_of = jax.random.split(jax.random.key(seed), 7)
    return {
        "inputs": scatter_about(streams_of[0], (TOKENS, D), 1.0, 6.0, ((0, 64),)),
        "query_cot": scatter_about(streams_of[1], (TOKENS, NQ), (1.0 / (TOK_DEV * N_FS) ** 0.5), 0.046875, ((0, 64), (1, 8))),
        "query_basis": scatter_about(streams_of[2], (D, RANK), D ** -0.5, 0.125, ((0, 64),)),
        "query_master": scatter_about(streams_of[3], (D, NQ), 0.5, 3.0, ((0, 64), (1, 8)), jnp.float32),
        "query_first": scatter_about(streams_of[4], (RANK, NQ), 1.0, 4.0, ((0, 64), (1, 8)), jnp.float32),
        "query_second": jnp.clip(jnp.exp(math.log(4.0) - 5.2983174 * jax.random.uniform(streams_of[5], (RANK, NQ), jnp.float32) ** levels(streams_of[5], (RANK, NQ), ((0, 64), (1, 8)), -0.2, 0.2)), 0.02, 4.0),
    }


def moments(first, second, low_grad):
    first_new = 0.8 * first + 0.2 * low_grad
    second_new = 0.9 * second + 0.1 * low_grad * low_grad
    return (first_new, second_new, first_new / jnp.sqrt(second_new))

def scaled(update, width):
    shaped = update.reshape(RANK, HEADS, width)
    head_mean = lax.optimization_barrier(jnp.mean(shaped * shaped, axis=(0, 2)))
    whole_mean = jnp.mean(update * update)
    factor = 1.0 / jnp.sqrt(head_mean + whole_mean)
    return (shaped * factor[None, :, None]).reshape(RANK, HEADS * width)

def reference(inputs, query_cot, query_basis, query_master, query_first, query_second):
    gradient = jnp.dot(inputs.T, query_cot, preferred_element_type=jnp.float32)
    basis_wide = query_basis.astype(jnp.float32)
    low_grad = jnp.dot(basis_wide.T, gradient, precision=lax.Precision.HIGHEST)
    first_new, second_new, update = moments(query_first, query_second, low_grad)
    step_full = jnp.dot(basis_wide, scaled(update, DQK), precision=lax.Precision.HIGHEST)
    copy_new = (query_master + step_full).astype(jnp.bfloat16)
    return (step_full, first_new, second_new, copy_new)
```

```python
import jax
import jax.numpy as jnp
from jax import lax
from jax.experimental import pallas as pl
from jax.experimental.pallas import tpu as pltpu
from jax.sharding import Mesh
from jax.sharding import PartitionSpec as P

HEADS = 8
DQK = 128
RANK = 256
NZ, NY, NX, NC = 16, 4, 4, 2
TP = ("x", "c")
FS = ("z", "y")
PLANE = ("y", "x", "c")
PER = RANK // HEADS
KEPT = 24

F32 = jnp.float32
BF16 = jnp.bfloat16


def vmem(count):
    return [pl.BlockSpec(memory_space=pltpu.VMEM)] * count


def call(kernel, out, operands, scalars=(), scratch=(), flops=200_000, limit=4 << 20):
    single = not isinstance(out, (list, tuple))
    moved = sum(a.size * a.dtype.itemsize for a in operands)
    return pl.pallas_call(
        kernel,
        out_shape=out,
        in_specs=[pl.BlockSpec(memory_space=pltpu.SMEM)] * len(scalars) + vmem(len(operands)),
        out_specs=vmem(1)[0] if single else vmem(len(out)),
        scratch_shapes=list(scratch),
        cost_estimate=pl.CostEstimate(flops=flops, bytes_accessed=moved, transcendentals=0),
        compiler_params=pltpu.CompilerParams(vmem_limit_bytes=limit),
    )(*scalars, *operands)


def exchange(parts, axes):
    return lax.all_to_all(parts, axes, 0, 0, tiled=True)


def pick_kernel(place, basis, out):
    j = place[0]
    rank = lax.broadcasted_iota(jnp.int32, (RANK, PER), 0)
    slot = lax.broadcasted_iota(jnp.int32, (RANK, PER), 1)
    wanted = (slot // 2) * (RANK // NZ) + 2 * j + slot % 2
    chosen = (rank == wanted).astype(F32).astype(BF16)
    mine = jnp.dot(basis[...], chosen, preferred_element_type=F32)
    wide = jnp.concatenate([mine[8 * q : 8 * q + 8] for q in range(4)], axis=1)
    out[...] = jnp.broadcast_to(wide.astype(BF16)[None], out.shape)


def project_kernel(place, inputs, columns, own, other, out):
    x, c = place[1], place[2]
    got = columns[...].astype(F32)
    basis = jnp.concatenate([got[:, :, PER * q : PER * q + PER] for q in range(4)], axis=1)
    basis = basis.reshape(inputs.shape[1], PER).astype(BF16)
    low = jnp.dot(inputs[...], basis, preferred_element_type=F32)
    high = low.astype(BF16)
    rest = (low - high.astype(F32)).astype(BF16)
    both = jnp.concatenate([high.astype(F32).T, rest.astype(F32).T], axis=0).astype(BF16)
    for cots, core in ((own, c), (other, 1 - c)):
        for s in range(NX):
            part = jnp.dot(both, cots[s], preferred_element_type=F32)
            part = part[:PER] + part[PER:]
            row = 4 * lax.rem(x + NX - s, NX) + 2 * core
            for z in range(NZ):
                out[z, pl.ds(row, 2), :] = part[2 * z : 2 * z + 2]


def sum_kernel(parts, first, second, out):
    shape = (NY * HEADS, 2 * HEADS, DQK)
    out[:, : 2 * HEADS, :] = jnp.broadcast_to(jnp.sum(parts[...], axis=0)[None], shape)
    pair = jnp.concatenate([first[...], second[...]], axis=0)
    out[:, 2 * HEADS :, :] = jnp.broadcast_to(pair[None], (NY * HEADS, 8, DQK))


def moments_kernel(place, parts, out, first_own, second_own, fn, sn, un):
    j, y = place[0], place[3]
    low = jnp.sum(parts[:, : 2 * HEADS, :].reshape(NY, HEADS, 2 * HEADS, DQK), axis=0)

    def moment(start):
        rows = []
        for i in range(2):
            at = start + 2 * i
            one = [
                jnp.concatenate([parts[b * HEADS + h, at : at + 2, :] for h in range(HEADS)], axis=0)
                for b in range(NY)
            ]
            rows.append(jnp.stack(one))
        return jnp.stack(rows, axis=1).reshape(HEADS, 2 * HEADS, DQK)

    first_new = 0.8 * moment(2 * HEADS) + 0.2 * low
    second_new = 0.9 * moment(2 * HEADS + 4) + 0.1 * low * low
    update = first_new / jnp.sqrt(second_new)
    fn[...] = first_new
    sn[...] = second_new
    un[...] = update
    rows = pl.ds(2 * j, 2)
    for i in range(2):
        first_own[2 * i : 2 * i + 2, :] = fn[2 * y + i, rows, :]
        second_own[2 * i : 2 * i + 2, :] = sn[2 * y + i, rows, :]
    total = jnp.sum(jnp.sum(update * update, axis=(0, 1), keepdims=True), axis=2, keepdims=True)
    own = jnp.concatenate([un[i, rows, :] for i in range(HEADS)], axis=0)
    out[:, : 2 * HEADS, :] = jnp.broadcast_to(own[None], (NZ, 2 * HEADS, DQK))
    out[:, 2 * HEADS :, :] = jnp.broadcast_to(total, (NZ, 8, DQK))


def step_kernel(parts, basis, master, step_out, copy_out):
    update = parts[:, : 2 * HEADS, :].reshape(RANK, DQK)
    whole = jnp.sum(parts[:, 2 * HEADS, :], axis=0, keepdims=True) / (RANK * HEADS * DQK)
    squares = jnp.sum(update * update, axis=0, keepdims=True)
    head = jnp.sum(squares, axis=1, keepdims=True) / (RANK * DQK)
    factor = 1.0 / jnp.sqrt(head + whole)
    high = update.astype(BF16)
    left = update - high.astype(F32)
    mid = left.astype(BF16)
    small = (left - mid.astype(F32)).astype(BF16)
    rows = basis[...]
    step = jnp.dot(rows, small, preferred_element_type=F32)
    step += jnp.dot(rows, mid, preferred_element_type=F32)
    step += jnp.dot(rows, high, preferred_element_type=F32)
    step *= factor
    step_out[...] = step
    copy_out[...] = (master[...] + step).astype(BF16)


def rotated(shard, axis, by):
    size = lax.axis_size(axis)
    return lax.ppermute(shard, axis, [(i, (i + by) % size) for i in range(size)])


def whole(inputs, query_cot, query_basis, query_master, query_first, query_second):
    sds = jax.ShapeDtypeStruct
    at = [lax.axis_index(axis) for axis in (TP, "x", "c", "y")]
    place = jnp.stack(at).astype(jnp.int32)
    picked = call(pick_kernel, sds((NZ * NY, 8, DQK), BF16), (query_basis,), (place,))
    columns = exchange(picked, FS)
    own = jnp.stack([query_cot] + [rotated(query_cot, "x", s) for s in range(1, NX)])
    other = rotated(own, "c", 1)
    low = call(
        project_kernel,
        sds((NZ, 2 * HEADS, DQK), F32),
        (inputs, columns, own, other),
        (place,),
        flops=400_000_000,
        limit=16 << 20,
    )
    low = exchange(low, "z")
    low = call(sum_kernel, sds((NY * HEADS, KEPT, DQK), F32), (low, query_first, query_second))
    low = exchange(low, PLANE)
    small = sds(query_first.shape, F32)
    update, first_new, second_new = call(
        moments_kernel,
        (sds((NZ, KEPT, DQK), F32), small, small),
        (low,),
        (place,),
        scratch=[pltpu.VMEM((HEADS, 2 * HEADS, DQK), F32)] * 3,
    )
    update = exchange(update, "z")
    step, copy = call(
        step_kernel,
        (sds(query_master.shape, F32), sds(query_master.shape, BF16)),
        (update, query_basis, query_master),
    )
    return (step, first_new, second_new, copy)


def solution(mesh):
    torus = Mesh(mesh.devices.reshape(NZ, NY, NX, NC), ("z", "y", "x", "c"))
    in_specs = (P(FS, None), P(FS, TP), P(FS, None), P(FS, TP), P(FS, TP), P(FS, TP))
    out_specs = (P(FS, TP), P(FS, TP), P(FS, TP), P(FS, TP))
    return jax.shard_map(whole, mesh=torus, in_specs=in_specs, out_specs=out_specs, check_vma=False)
```

```python
import jax
import jax.numpy as jnp
from jax import lax
from jax.experimental import pallas as pl
from jax.experimental.pallas import tpu as pltpu
from jax.sharding import Mesh
from jax.sharding import PartitionSpec as P

HEADS = 8
DQK = 128
RANK = 256
ZH, ZL, NY, NX, NC = 8, 2, 4, 4, 2
TP = ("x", "c")
FS = ("zh", "zl", "y")
NEAR = ("zl", "y")
GROUPS = ZL * NY
PER = RANK // GROUPS
OWN = PER // ZH

F32 = jnp.float32
BF16 = jnp.bfloat16


def vmem(count):
    return [pl.BlockSpec(memory_space=pltpu.VMEM)] * count


def call(kernel, out, operands, scalars=(), scratch=(), specs=None, flops=200_000, limit=4 << 20, name=None):
    single = not isinstance(out, (list, tuple))
    moved = sum(a.size * a.dtype.itemsize for a in operands)
    return pl.pallas_call(
        kernel,
        out_shape=out,
        in_specs=[pl.BlockSpec(memory_space=pltpu.SMEM)] * len(scalars) + (specs or vmem(len(operands))),
        out_specs=vmem(1)[0] if single else vmem(len(out)),
        scratch_shapes=list(scratch),
        cost_estimate=pl.CostEstimate(flops=flops, bytes_accessed=moved, transcendentals=0),
        compiler_params=pltpu.CompilerParams(vmem_limit_bytes=limit),
        name=name,
    )(*scalars, *operands)


def exchange(parts, axes, name):
    with jax.named_scope(name):
        return lax.all_to_all(parts, axes, 0, 0, tiled=True)


def copies(block, count):
    return jnp.broadcast_to(block[None], (count, *block.shape))


def pick_kernel(place, inputs, basis, out, held, rows, sems):
    near = pltpu.make_async_copy(basis, rows, sems.at[0])
    far = pltpu.make_async_copy(inputs, held, sems.at[1])
    near.start()
    far.start()
    rank = lax.broadcasted_iota(jnp.int32, (RANK, PER), 0)
    slot = lax.broadcasted_iota(jnp.int32, (RANK, PER), 1)
    wanted = (slot // OWN) * PER + OWN * place[0] + slot % OWN
    chosen = (rank == wanted).astype(F32).astype(BF16)
    near.wait()
    mine = jnp.dot(rows[...], chosen, preferred_element_type=F32)
    wide = jnp.concatenate([mine[8 * q : 8 * q + 8] for q in range(4)], axis=1)
    out[...] = copies(wide.astype(BF16), out.shape[0])
    far.wait()


def project_kernel(inputs, columns, out):
    got = columns[...].astype(F32)
    basis = jnp.concatenate([got[:, :, PER * q : PER * q + PER] for q in range(4)], axis=1)
    basis = basis.reshape(inputs.shape[1], PER).astype(BF16)
    low = jnp.dot(inputs[...], basis, preferred_element_type=F32)
    high = low.astype(BF16)
    rest = (low - high.astype(F32)).astype(BF16)
    both = jnp.concatenate([high.astype(F32).T, rest.astype(F32).T], axis=0).astype(BF16)
    out[...] = copies(both, out.shape[0])


def low_kernel(both, cot, out):
    low = both[...].reshape(GROUPS * 2 * PER, both.shape[2])
    low = jnp.dot(low, cot[...], preferred_element_type=F32).reshape(GROUPS, 2 * PER, DQK)
    out[...] = low[:, :PER] + low[:, PER:]


def sum_kernel(parts, first, second, out):
    out[:, :PER, :] = copies(jnp.sum(parts[...], axis=0), ZH)
    pair = jnp.concatenate([first[...], second[...]], axis=0)
    out[:, PER:, :] = copies(pair, ZH)


def moments_kernel(place, parts, out, first_own, second_own, fn, sn):
    low = jnp.sum(parts[:, :PER, :], axis=0)
    first = jnp.concatenate([parts[z, PER : PER + OWN, :] for z in range(ZH)], axis=0)
    second = jnp.concatenate([parts[z, PER + OWN : PER + 2 * OWN, :] for z in range(ZH)], axis=0)
    first_new = 0.8 * first + 0.2 * low
    second_new = 0.9 * second + 0.1 * low * low
    fn[...] = first_new
    sn[...] = second_new
    out[...] = copies(first_new / jnp.sqrt(second_new), GROUPS)
    rows = pl.ds(OWN * place[1], OWN)
    first_own[...] = fn[rows, :]
    second_own[...] = sn[rows, :]


def apply_kernel(parts, basis, squares_out, step_out):
    update = jnp.concatenate(
        [parts[g, OWN * z : OWN * (z + 1), :] for z in range(ZH) for g in range(GROUPS)], axis=0
    )
    squares = jnp.sum(jnp.sum(update * update, axis=0, keepdims=True), axis=1, keepdims=True)
    squares_out[...] = jnp.broadcast_to(squares[None], squares_out.shape)
    high = update.astype(BF16)
    left = update - high.astype(F32)
    mid = left.astype(BF16)
    small = (left - mid.astype(F32)).astype(BF16)
    rows = basis[...]
    step = jnp.dot(rows, small, preferred_element_type=F32)
    step += jnp.dot(rows, mid, preferred_element_type=F32)
    step_out[...] = step + jnp.dot(rows, high, preferred_element_type=F32)


def scale_kernel(squares, own, raw, master, first, second, step_out, first_out, second_out, copy_out):
    whole = jnp.sum(squares[...], axis=0) / (RANK * HEADS * DQK)
    head = own[0] / (RANK * DQK)
    step = raw[...] * (1.0 / jnp.sqrt(head + whole))
    step_out[...] = step
    copy_out[...] = (master[...] + step).astype(BF16)
    first_out[...] = first[...]
    second_out[...] = second[...]


def body(inputs, query_cot, query_basis, query_master, query_first, query_second):
    sds = jax.ShapeDtypeStruct
    place = jnp.stack([lax.axis_index(TP), lax.axis_index("zh")]).astype(jnp.int32)
    tokens, small = inputs.shape[0], sds(query_first.shape, F32)
    columns, held = call(
        pick_kernel,
        (sds((ZH * GROUPS, 8, DQK), BF16), sds(inputs.shape, BF16)),
        (inputs, query_basis),
        (place,),
        specs=[pl.BlockSpec(memory_space=pltpu.HBM)] * 2,
        scratch=[pltpu.VMEM(query_basis.shape, BF16), pltpu.SemaphoreType.DMA((2,))],
        name="pick",
    )
    columns = exchange(columns, FS, "columns")
    both = call(
        project_kernel,
        sds((GROUPS, 2 * PER, tokens), BF16),
        (held, columns),
        flops=400_000_000,
        limit=16 << 20,
        name="project",
    )
    both = exchange(both, TP, "ranks")
    low = call(low_kernel, sds((GROUPS, PER, DQK), F32), (both, query_cot), name="low")
    low = exchange(low, NEAR, "near_sum")
    low = call(
        sum_kernel,
        sds((ZH, PER + 2 * OWN, DQK), F32),
        (low, query_first, query_second),
        name="sum_near",
    )
    low = exchange(low, "zh", "far_sum")
    update, first_new, second_new = call(
        moments_kernel,
        (sds((GROUPS, PER, DQK), F32), small, small),
        (low,),
        (place,),
        scratch=[pltpu.VMEM((PER, DQK), F32)] * 2,
        name="moments",
    )
    update = exchange(update, NEAR, "updates")
    squares, step = call(
        apply_kernel,
        (sds((HEADS, 1, DQK), F32), sds(query_master.shape, F32)),
        (update, query_basis),
        name="apply",
    )
    heads = exchange(squares, TP, "squares")
    step, first_new, second_new, copy = call(
        scale_kernel,
        (sds(query_master.shape, F32), small, small, sds(query_master.shape, BF16)),
        (heads, squares, step, query_master, first_new, second_new),
        name="scale",
    )
    return (step, first_new, second_new, copy)


def solution(mesh):
    torus = Mesh(mesh.devices.reshape(ZH, ZL, NY, NX, NC), (*FS, *TP))
    in_specs = (P(FS, None), P(FS, TP), P(FS, None), P(FS, TP), P(FS, TP), P(FS, TP))
    out_specs = (P(FS, TP), P(FS, TP), P(FS, TP), P(FS, TP))
    return jax.shard_map(body, mesh=torus, in_specs=in_specs, out_specs=out_specs, check_vma=False)
```

```python
import jax
import jax.numpy as jnp
from jax import lax
from jax.experimental import pallas as pl
from jax.experimental.pallas import tpu as pltpu
from jax.sharding import Mesh
from jax.sharding import PartitionSpec as P

HEADS = 8
DQK = 128
RANK = 256
ZH, ZL, NY, NX, NC = 8, 2, 4, 4, 2
TP = ("x", "c")
FS = ("zh", "zl", "y")
NEAR = ("zl", "y")
GROUPS = ZL * NY
PER = RANK // GROUPS
OWN = PER // ZH
FIRST_ROWS = 46
FIRST_ZH = 5
FIRST_RANKS = 5
FIRST_SUM = 6
FIRST_UPDATES = 6
FIRST_SQUARES = 5

F32 = jnp.float32
BF16 = jnp.bfloat16


def vmem(count):
    return [pl.BlockSpec(memory_space=pltpu.VMEM)] * count


def call(kernel, out, operands, scalars=(), scratch=(), specs=None, flops=200_000, limit=4 << 20, name=None):
    single = not isinstance(out, (list, tuple))
    moved = sum(a.size * a.dtype.itemsize for a in operands)
    return pl.pallas_call(
        kernel,
        out_shape=out,
        in_specs=[pl.BlockSpec(memory_space=pltpu.SMEM)] * len(scalars) + (specs or vmem(len(operands))),
        out_specs=vmem(1)[0] if single else vmem(len(out)),
        scratch_shapes=list(scratch),
        cost_estimate=pl.CostEstimate(flops=flops, bytes_accessed=moved, transcendentals=0),
        compiler_params=pltpu.CompilerParams(vmem_limit_bytes=limit),
        name=name,
    )(*scalars, *operands)


def exchange(parts, axes, name, first=0):
    count = parts.shape[0]
    groups = [[(first + i) % count for i in range(count)]] if first else None
    with jax.named_scope(name):
        return lax.all_to_all(parts, axes, 0, 0, axis_index_groups=groups, tiled=True)


def in_turn(blocks, first):
    count = len(blocks)
    return [blocks[(i - first) % count] for i in range(count)]


def copies(block, count):
    return jnp.broadcast_to(block[None], (count, *block.shape))


def pick_kernel(place, inputs, basis, out, held, sem):
    fetch = pltpu.make_async_copy(inputs, held, sem)
    fetch.start()
    rank = lax.broadcasted_iota(jnp.int32, (RANK, PER), 0)
    slot = lax.broadcasted_iota(jnp.int32, (RANK, PER), 1)
    wanted = (slot // OWN) * PER + OWN * place[0] + slot % OWN
    chosen = (rank == wanted).astype(F32).astype(BF16)
    mine = jnp.dot(basis[...], chosen, preferred_element_type=F32)
    wide = jnp.concatenate([mine[8 * q : 8 * q + 8] for q in range(4)], axis=1)
    out[...] = copies(wide.astype(BF16), out.shape[0])
    fetch.wait()


def project_kernel(inputs, columns, out):
    got = columns[...].astype(F32)
    if FIRST_ROWS:
        got = jnp.concatenate([got[-FIRST_ROWS:], got[:-FIRST_ROWS]], axis=0)
    basis = jnp.concatenate([got[:, :, PER * q : PER * q + PER] for q in range(4)], axis=1)
    basis = basis.reshape(inputs.shape[1], PER).astype(BF16)
    low = jnp.dot(inputs[...], basis, preferred_element_type=F32)
    high = low.astype(BF16)
    rest = (low - high.astype(F32)).astype(BF16)
    both = jnp.concatenate([high.astype(F32).T, rest.astype(F32).T], axis=0).astype(BF16)
    out[...] = copies(both, out.shape[0])


def low_kernel(both, cot, out):
    low = both[...].reshape(GROUPS * 2 * PER, both.shape[2])
    low = jnp.dot(low, cot[...], preferred_element_type=F32).reshape(GROUPS, 2 * PER, DQK)
    low = low[:, :PER] + low[:, PER:]
    for g in range(GROUPS):
        out[(g - FIRST_SUM) % GROUPS] = low[(g - FIRST_RANKS) % GROUPS]


def sum_kernel(parts, first, second, out):
    out[:, :PER, :] = copies(jnp.sum(parts[...], axis=0), ZH)
    pair = jnp.concatenate([first[...], second[...]], axis=0)
    out[:, PER:, :] = copies(pair, ZH)


def moments_kernel(place, parts, out, first_own, second_own, fn, sn):
    low = jnp.sum(parts[:, :PER, :], axis=0)
    first = [parts[z, PER : PER + OWN, :] for z in range(ZH)]
    first = jnp.concatenate(in_turn(first, FIRST_ZH), axis=0)
    second = [parts[z, PER + OWN : PER + 2 * OWN, :] for z in range(ZH)]
    second = jnp.concatenate(in_turn(second, FIRST_ZH), axis=0)
    first_new = 0.8 * first + 0.2 * low
    second_new = 0.9 * second + 0.1 * low * low
    fn[...] = first_new
    sn[...] = second_new
    out[...] = copies(first_new / jnp.sqrt(second_new), GROUPS)
    rows = pl.ds(OWN * place[1], OWN)
    first_own[...] = fn[rows, :]
    second_own[...] = sn[rows, :]


def apply_kernel(parts, basis, squares_out, step_out):
    update = jnp.concatenate(
        [
            parts[(g - FIRST_UPDATES) % GROUPS, OWN * z : OWN * (z + 1), :]
            for z in range(ZH)
            for g in range(GROUPS)
        ],
        axis=0,
    )
    squares = jnp.sum(jnp.sum(update * update, axis=0, keepdims=True), axis=1, keepdims=True)
    squares_out[...] = jnp.broadcast_to(squares[None], squares_out.shape)
    high = update.astype(BF16)
    left = update - high.astype(F32)
    mid = left.astype(BF16)
    small = (left - mid.astype(F32)).astype(BF16)
    rows = basis[...]
    step = jnp.dot(rows, small, preferred_element_type=F32)
    step += jnp.dot(rows, mid, preferred_element_type=F32)
    step_out[...] = step + jnp.dot(rows, high, preferred_element_type=F32)


def scale_kernel(squares, own, raw, master, first, second, step_out, first_out, second_out, copy_out):
    whole = jnp.sum(squares[...], axis=0) / (RANK * HEADS * DQK)
    head = own[0] / (RANK * DQK)
    step = raw[...] * (1.0 / jnp.sqrt(head + whole))
    step_out[...] = step
    copy_out[...] = (master[...] + step).astype(BF16)
    first_out[...] = first[...]
    second_out[...] = second[...]


def body(inputs, query_cot, query_basis, query_master, query_first, query_second):
    sds = jax.ShapeDtypeStruct
    place = jnp.stack([lax.axis_index(TP), lax.axis_index("zh")]).astype(jnp.int32)
    tokens, small = inputs.shape[0], sds(query_first.shape, F32)
    columns, held = call(
        pick_kernel,
        (sds((ZH * GROUPS, 8, DQK), BF16), sds(inputs.shape, BF16)),
        (inputs, query_basis),
        (place,),
        specs=[pl.BlockSpec(memory_space=pltpu.HBM), *vmem(1)],
        scratch=[pltpu.SemaphoreType.DMA],
        limit=54000 << 10,
        name="pick",
    )
    columns = exchange(columns, FS, "columns", FIRST_ROWS)
    both = call(
        project_kernel,
        sds((GROUPS, 2 * PER, tokens), BF16),
        (held, columns),
        flops=400_000_000,
        limit=16 << 20,
        name="project",
    )
    both = exchange(both, TP, "ranks", FIRST_RANKS)
    low = call(low_kernel, sds((GROUPS, PER, DQK), F32), (both, query_cot), name="low")
    low = exchange(low, NEAR, "near_sum", FIRST_SUM)
    low = call(
        sum_kernel,
        sds((ZH, PER + 2 * OWN, DQK), F32),
        (low, query_first, query_second),
        name="sum_near",
    )
    low = exchange(low, "zh", "far_sum", FIRST_ZH)
    update, first_new, second_new = call(
        moments_kernel,
        (sds((GROUPS, PER, DQK), F32), small, small),
        (low,),
        (place,),
        scratch=[pltpu.VMEM((PER, DQK), F32)] * 2,
        name="moments",
    )
    update = exchange(update, NEAR, "updates", FIRST_UPDATES)
    squares, step = call(
        apply_kernel,
        (sds((HEADS, 1, DQK), F32), sds(query_master.shape, F32)),
        (update, query_basis),
        name="apply",
    )
    heads = exchange(squares, TP, "squares", FIRST_SQUARES)
    step, first_new, second_new, copy = call(
        scale_kernel,
        (sds(query_master.shape, F32), small, small, sds(query_master.shape, BF16)),
        (heads, squares, step, query_master, first_new, second_new),
        name="scale",
    )
    return (step, first_new, second_new, copy)


def solution(mesh):
    torus = Mesh(mesh.devices.reshape(ZH, ZL, NY, NX, NC), (*FS, *TP))
    in_specs = (P(FS, None), P(FS, TP), P(FS, None), P(FS, TP), P(FS, TP), P(FS, TP))
    out_specs = (P(FS, TP), P(FS, TP), P(FS, TP), P(FS, TP))
    return jax.shard_map(body, mesh=torus, in_specs=in_specs, out_specs=out_specs, check_vma=False)
```

```python
import jax
import jax.numpy as jnp
from jax import lax
from jax.experimental import pallas as pl
from jax.experimental.pallas import tpu as pltpu
from jax.sharding import Mesh
from jax.sharding import PartitionSpec as P

HEADS = 8
DQK = 128
RANK = 256
ZH, ZL, NY, NX, NC = 8, 2, 4, 4, 2
TP = ("x", "c")
FS = ("zh", "zl", "y")
NEAR = ("zl", "y")
GROUPS = ZL * NY
PER = RANK // GROUPS
OWN = PER // ZH
FETCHES = 2
FIRST_ROWS = 46
FIRST_ZH = 5
FIRST_RANKS = 5
FIRST_SUM = 6
FIRST_UPDATES = 6
FIRST_SQUARES = 5

F32 = jnp.float32
BF16 = jnp.bfloat16


def vmem(count):
    return [pl.BlockSpec(memory_space=pltpu.VMEM)] * count


def call(kernel, out, operands, scalars=(), scratch=(), specs=None, flops=200_000, limit=4 << 20, name=None):
    single = not isinstance(out, (list, tuple))
    moved = sum(a.size * a.dtype.itemsize for a in operands)
    return pl.pallas_call(
        kernel,
        out_shape=out,
        in_specs=[pl.BlockSpec(memory_space=pltpu.SMEM)] * len(scalars) + (specs or vmem(len(operands))),
        out_specs=vmem(1)[0] if single else vmem(len(out)),
        scratch_shapes=list(scratch),
        cost_estimate=pl.CostEstimate(flops=flops, bytes_accessed=moved, transcendentals=0),
        compiler_params=pltpu.CompilerParams(vmem_limit_bytes=limit),
        name=name,
    )(*scalars, *operands)


def exchange(parts, axes, name, first=0):
    count = parts.shape[0]
    groups = [[(first + i) % count for i in range(count)]] if first else None
    with jax.named_scope(name):
        return lax.all_to_all(parts, axes, 0, 0, axis_index_groups=groups, tiled=True)


def in_turn(blocks, first):
    count = len(blocks)
    return [blocks[(i - first) % count] for i in range(count)]


def copies(block, count):
    return jnp.broadcast_to(block[None], (count, *block.shape))


def pick_kernel(inputs, basis, out, held, rows, sems):
    near = pltpu.make_async_copy(basis, rows, sems.at[0])
    near.start()
    fetches = []
    for i in range(FETCHES):
        part = pl.ds(i * (held.shape[0] // FETCHES), held.shape[0] // FETCHES)
        fetches.append(pltpu.make_async_copy(inputs.at[part], held.at[part], sems.at[1 + i]))
    for fetch in fetches:
        fetch.start()
    rank = lax.broadcasted_iota(jnp.int32, (RANK, PER), 0)
    slot = lax.broadcasted_iota(jnp.int32, (RANK, PER), 1)
    wanted = (slot // OWN) * PER + OWN * lax.axis_index(TP) + slot % OWN
    chosen = (rank == wanted).astype(F32).astype(BF16)
    near.wait()
    mine = jnp.dot(rows[...], chosen, preferred_element_type=F32)
    wide = jnp.concatenate([mine[8 * q : 8 * q + 8] for q in range(4)], axis=1)
    out[...] = copies(wide.astype(BF16), out.shape[0])
    for fetch in fetches:
        fetch.wait()


def project_kernel(inputs, columns, out):
    got = columns[...].astype(F32)
    if FIRST_ROWS:
        got = jnp.concatenate([got[-FIRST_ROWS:], got[:-FIRST_ROWS]], axis=0)
    lane = lax.broadcasted_iota(jnp.int32, got.shape, 2) // PER
    basis = jnp.concatenate([jnp.where(lane == q, got, 0.0) for q in range(4)], axis=1)
    basis = basis.reshape(inputs.shape[1], DQK).astype(BF16)
    low = jnp.dot(inputs[...], basis, preferred_element_type=F32).T
    low = (low[:PER] + low[PER : 2 * PER]) + (low[2 * PER : 3 * PER] + low[3 * PER :])
    high = low.astype(BF16)
    rest = (low - high.astype(F32)).astype(BF16)
    out[...] = copies(jnp.concatenate([high, rest], axis=0), out.shape[0])


def low_kernel(both, cot, out):
    low = both[...].reshape(GROUPS * 2 * PER, both.shape[2])
    low = jnp.dot(low, cot[...], preferred_element_type=F32).reshape(GROUPS, 2 * PER, DQK)
    low = low[:, :PER] + low[:, PER:]
    for g in range(GROUPS):
        out[(g - FIRST_SUM) % GROUPS] = low[(g - FIRST_RANKS) % GROUPS]


def sum_kernel(parts, first, second, out):
    out[:, :PER, :] = copies(jnp.sum(parts[...], axis=0), ZH)
    pair = jnp.concatenate([first[...], second[...]], axis=0)
    out[:, PER:, :] = copies(pair, ZH)


def moments_kernel(parts, out, first_own, second_own, fn, sn):
    low = jnp.sum(parts[:, :PER, :], axis=0)
    first = [parts[z, PER : PER + OWN, :] for z in range(ZH)]
    first = jnp.concatenate(in_turn(first, FIRST_ZH), axis=0)
    second = [parts[z, PER + OWN : PER + 2 * OWN, :] for z in range(ZH)]
    second = jnp.concatenate(in_turn(second, FIRST_ZH), axis=0)
    first_new = 0.8 * first + 0.2 * low
    second_new = 0.9 * second + 0.1 * low * low
    fn[...] = first_new
    sn[...] = second_new
    out[...] = copies(first_new / jnp.sqrt(second_new), GROUPS)
    rows = pl.ds(OWN * lax.axis_index("zh"), OWN)
    first_own[...] = fn[rows, :]
    second_own[...] = sn[rows, :]


def apply_kernel(parts, basis, squares_out, step_out):
    update = jnp.concatenate(
        [
            parts[(g - FIRST_UPDATES) % GROUPS, OWN * z : OWN * (z + 1), :]
            for z in range(ZH)
            for g in range(GROUPS)
        ],
        axis=0,
    )
    squares = jnp.sum(jnp.sum(update * update, axis=0, keepdims=True), axis=1, keepdims=True)
    squares_out[...] = jnp.broadcast_to(squares[None], squares_out.shape)
    high = update.astype(BF16)
    left = update - high.astype(F32)
    mid = left.astype(BF16)
    small = (left - mid.astype(F32)).astype(BF16)
    rows = basis[...]
    step = jnp.dot(rows, small, preferred_element_type=F32)
    step += jnp.dot(rows, mid, preferred_element_type=F32)
    step_out[...] = step + jnp.dot(rows, high, preferred_element_type=F32)


def scale_kernel(squares, own, raw, master, first, second, step_out, first_out, second_out, copy_out):
    whole = jnp.sum(squares[...], axis=0) / (RANK * HEADS * DQK)
    head = own[0] / (RANK * DQK)
    step = raw[...] * (1.0 / jnp.sqrt(head + whole))
    step_out[...] = step
    copy_out[...] = (master[...] + step).astype(BF16)
    first_out[...] = first[...]
    second_out[...] = second[...]


def body(inputs, query_cot, query_basis, query_master, query_first, query_second):
    sds = jax.ShapeDtypeStruct
    tokens, small = inputs.shape[0], sds(query_first.shape, F32)
    columns, held = call(
        pick_kernel,
        (sds((ZH * GROUPS, 8, DQK), BF16), sds(inputs.shape, BF16)),
        [pltpu.with_memory_space_constraint(a, pltpu.HBM) for a in (inputs, query_basis)],
        specs=[pl.BlockSpec(memory_space=pltpu.HBM)] * 2,
        scratch=[pltpu.VMEM(query_basis.shape, BF16), pltpu.SemaphoreType.DMA((1 + FETCHES,))],
        limit=4 << 20,
        name="pick",
    )
    columns = exchange(columns, FS, "columns", FIRST_ROWS)
    both = call(
        project_kernel,
        sds((GROUPS, 2 * PER, tokens), BF16),
        (held, columns),
        flops=400_000_000,
        limit=16 << 20,
        name="project",
    )
    both = exchange(both, TP, "ranks", FIRST_RANKS)
    low = call(low_kernel, sds((GROUPS, PER, DQK), F32), (both, query_cot), name="low")
    low = exchange(low, NEAR, "near_sum", FIRST_SUM)
    low = call(
        sum_kernel,
        sds((ZH, PER + 2 * OWN, DQK), F32),
        (low, query_first, query_second),
        name="sum_near",
    )
    low = exchange(low, "zh", "far_sum", FIRST_ZH)
    update, first_new, second_new = call(
        moments_kernel,
        (sds((GROUPS, PER, DQK), F32), small, small),
        (low,),
        scratch=[pltpu.VMEM((PER, DQK), F32)] * 2,
        name="moments",
    )
    update = exchange(update, NEAR, "updates", FIRST_UPDATES)
    squares, step = call(
        apply_kernel,
        (sds((HEADS, 1, DQK), F32), sds(query_master.shape, F32)),
        (update, query_basis),
        name="apply",
    )
    heads = exchange(squares, TP, "squares", FIRST_SQUARES)
    step, first_new, second_new, copy = call(
        scale_kernel,
        (sds(query_master.shape, F32), small, small, sds(query_master.shape, BF16)),
        (heads, squares, step, query_master, first_new, second_new),
        name="scale",
    )
    return (step, first_new, second_new, copy)


def solution(mesh):
    torus = Mesh(mesh.devices.reshape(ZH, ZL, NY, NX, NC), (*FS, *TP))
    in_specs = (P(FS, None), P(FS, TP), P(FS, None), P(FS, TP), P(FS, TP), P(FS, TP))
    out_specs = (P(FS, TP), P(FS, TP), P(FS, TP), P(FS, TP))
    return jax.shard_map(body, mesh=torus, in_specs=in_specs, out_specs=out_specs, check_vma=False)
```

```python
import jax
import jax.numpy as jnp
from jax import lax
from jax.experimental import pallas as pl
from jax.experimental.pallas import tpu as pltpu
from jax.sharding import Mesh
from jax.sharding import PartitionSpec as P

HEADS = 8
DQK = 128
RANK = 256
ZH, ZL, NY, NX, NC = 8, 2, 4, 4, 2
TP = ("x", "c")
FS = ("zh", "zl", "y")
NEAR = ("zl", "y")
GROUPS = ZL * NY
PER = RANK // GROUPS
OWN = PER // ZH
FETCHES = 2
FIRST_ROWS = 46
FIRST_ZH = (5, 4)
FIRST_RANKS = 5
FIRST_SUM = 6
FIRST_UPDATES = 6
FIRST_SQUARES = 5

F32 = jnp.float32
BF16 = jnp.bfloat16


def vmem(count):
    return [pl.BlockSpec(memory_space=pltpu.VMEM)] * count


def call(kernel, out, operands, scalars=(), scratch=(), specs=None, flops=200_000, limit=4 << 20, name=None):
    single = not isinstance(out, (list, tuple))
    moved = sum(a.size * a.dtype.itemsize for a in operands)
    return pl.pallas_call(
        kernel,
        out_shape=out,
        in_specs=[pl.BlockSpec(memory_space=pltpu.SMEM)] * len(scalars) + (specs or vmem(len(operands))),
        out_specs=vmem(1)[0] if single else vmem(len(out)),
        scratch_shapes=list(scratch),
        cost_estimate=pl.CostEstimate(flops=flops, bytes_accessed=moved, transcendentals=0),
        compiler_params=pltpu.CompilerParams(vmem_limit_bytes=limit),
        name=name,
    )(*scalars, *operands)


def exchange(parts, axes, name, first=0):
    count = parts.shape[0]
    groups = [[(first + i) % count for i in range(count)]] if first else None
    with jax.named_scope(name):
        return lax.all_to_all(parts, axes, 0, 0, axis_index_groups=groups, tiled=True)


def copies(block, count):
    return jnp.broadcast_to(block[None], (count, *block.shape))


def pick_kernel(inputs, basis, out, held, rows, sems):
    near = pltpu.make_async_copy(basis, rows, sems.at[0])
    near.start()
    fetches = []
    for i in range(FETCHES):
        part = pl.ds(i * (held.shape[0] // FETCHES), held.shape[0] // FETCHES)
        fetches.append(pltpu.make_async_copy(inputs.at[part], held.at[part], sems.at[1 + i]))
    for fetch in fetches:
        fetch.start()
    rank = lax.broadcasted_iota(jnp.int32, (RANK, PER), 0)
    slot = lax.broadcasted_iota(jnp.int32, (RANK, PER), 1)
    wanted = (slot // OWN) * PER + OWN * lax.axis_index(TP) + slot % OWN
    chosen = (rank == wanted).astype(F32).astype(BF16)
    near.wait()
    mine = jnp.dot(rows[...], chosen, preferred_element_type=F32)
    wide = jnp.concatenate([mine[8 * q : 8 * q + 8] for q in range(4)], axis=1)
    out[...] = copies(wide.astype(BF16), out.shape[0])
    for fetch in fetches:
        fetch.wait()


def project_kernel(inputs, columns, out):
    got = columns[...].astype(F32)
    if FIRST_ROWS:
        got = jnp.concatenate([got[-FIRST_ROWS:], got[:-FIRST_ROWS]], axis=0)
    lane = lax.broadcasted_iota(jnp.int32, got.shape, 2) // PER
    basis = jnp.concatenate([jnp.where(lane == q, got, 0.0) for q in range(4)], axis=1)
    basis = basis.reshape(inputs.shape[1], DQK).astype(BF16)
    low = jnp.dot(inputs[...], basis, preferred_element_type=F32).T
    low = (low[:PER] + low[PER : 2 * PER]) + (low[2 * PER : 3 * PER] + low[3 * PER :])
    high = low.astype(BF16)
    rest = (low - high.astype(F32)).astype(BF16)
    out[...] = copies(jnp.concatenate([high, rest], axis=0), out.shape[0])


def low_kernel(both, cot, out):
    low = both[...].reshape(GROUPS * 2 * PER, both.shape[2])
    low = jnp.dot(low, cot[...], preferred_element_type=F32).reshape(GROUPS, 2 * PER, DQK)
    low = low[:, :PER] + low[:, PER:]
    for g in range(GROUPS):
        out[(g - FIRST_SUM) % GROUPS] = low[(g - FIRST_RANKS) % GROUPS]


def sum_kernel(parts, first, second, out):
    out[:, :PER, :] = copies(jnp.sum(parts[...], axis=0), ZH)
    pair = jnp.concatenate([first[...], second[...]], axis=0)
    out[:, PER:, :] = copies(pair, ZH)


def moments_kernel(parts, out, first_own, second_own, fn, sn):
    low = jnp.sum(parts[:, :PER, :], axis=0)
    start = jnp.where(lax.axis_index("zl") == 0, FIRST_ZH[0], FIRST_ZH[1])
    turn = [lax.rem(z + ZH - start, ZH) for z in range(ZH)]
    first = jnp.concatenate([parts[t, PER : PER + OWN, :] for t in turn], axis=0)
    second = jnp.concatenate([parts[t, PER + OWN : PER + 2 * OWN, :] for t in turn], axis=0)
    first_new = 0.8 * first + 0.2 * low
    second_new = 0.9 * second + 0.1 * low * low
    fn[...] = first_new
    sn[...] = second_new
    out[...] = copies(first_new / jnp.sqrt(second_new), GROUPS)
    rows = pl.ds(OWN * lax.axis_index("zh"), OWN)
    first_own[...] = fn[rows, :]
    second_own[...] = sn[rows, :]


def apply_kernel(parts, basis, squares_out, step_out):
    update = jnp.concatenate(
        [
            parts[(g - FIRST_UPDATES) % GROUPS, OWN * z : OWN * (z + 1), :]
            for z in range(ZH)
            for g in range(GROUPS)
        ],
        axis=0,
    )
    squares = jnp.sum(jnp.sum(update * update, axis=0, keepdims=True), axis=1, keepdims=True)
    squares_out[...] = jnp.broadcast_to(squares[None], squares_out.shape)
    high = update.astype(BF16)
    left = update - high.astype(F32)
    mid = left.astype(BF16)
    small = (left - mid.astype(F32)).astype(BF16)
    rows = basis[...]
    step = jnp.dot(rows, small, preferred_element_type=F32)
    step += jnp.dot(rows, mid, preferred_element_type=F32)
    step_out[...] = step + jnp.dot(rows, high, preferred_element_type=F32)


def scale_kernel(squares, own, raw, master, first, second, step_out, first_out, second_out, copy_out):
    whole = jnp.sum(squares[...], axis=0) / (RANK * HEADS * DQK)
    head = own[0] / (RANK * DQK)
    step = raw[...] * (1.0 / jnp.sqrt(head + whole))
    step_out[...] = step
    copy_out[...] = (master[...] + step).astype(BF16)
    first_out[...] = first[...]
    second_out[...] = second[...]


def body(inputs, query_cot, query_basis, query_master, query_first, query_second):
    sds = jax.ShapeDtypeStruct
    tokens, small = inputs.shape[0], sds(query_first.shape, F32)
    columns, held = call(
        pick_kernel,
        (sds((ZH * GROUPS, 8, DQK), BF16), sds(inputs.shape, BF16)),
        [pltpu.with_memory_space_constraint(a, pltpu.HBM) for a in (inputs, query_basis)],
        specs=[pl.BlockSpec(memory_space=pltpu.HBM)] * 2,
        scratch=[pltpu.VMEM(query_basis.shape, BF16), pltpu.SemaphoreType.DMA((1 + FETCHES,))],
        limit=4 << 20,
        name="pick",
    )
    columns = exchange(columns, FS, "columns", FIRST_ROWS)
    both = call(
        project_kernel,
        sds((GROUPS, 2 * PER, tokens), BF16),
        (held, columns),
        flops=400_000_000,
        limit=16 << 20,
        name="project",
    )
    both = exchange(both, TP, "ranks", FIRST_RANKS)
    low = call(low_kernel, sds((GROUPS, PER, DQK), F32), (both, query_cot), name="low")
    low = exchange(low, NEAR, "near_sum", FIRST_SUM)
    low = call(
        sum_kernel,
        sds((ZH, PER + 2 * OWN, DQK), F32),
        (low, query_first, query_second),
        name="sum_near",
    )
    groups = [[(FIRST_ZH[b] + i) % ZH * ZL + b for i in range(ZH)] for b in range(ZL)]
    with jax.named_scope("far_sum"):
        low = lax.all_to_all(low, ("zh", "zl"), 0, 0, axis_index_groups=groups, tiled=True)
    update, first_new, second_new = call(
        moments_kernel,
        (sds((GROUPS, PER, DQK), F32), small, small),
        (low,),
        scratch=[pltpu.VMEM((PER, DQK), F32)] * 2,
        name="moments",
    )
    update = exchange(update, NEAR, "updates", FIRST_UPDATES)
    squares, step = call(
        apply_kernel,
        (sds((HEADS, 1, DQK), F32), sds(query_master.shape, F32)),
        (update, query_basis),
        name="apply",
    )
    heads = exchange(squares, TP, "squares", FIRST_SQUARES)
    step, first_new, second_new, copy = call(
        scale_kernel,
        (sds(query_master.shape, F32), small, small, sds(query_master.shape, BF16)),
        (heads, squares, step, query_master, first_new, second_new),
        name="scale",
    )
    return (step, first_new, second_new, copy)


def solution(mesh):
    torus = Mesh(mesh.devices.reshape(ZH, ZL, NY, NX, NC), (*FS, *TP))
    in_specs = (P(FS, None), P(FS, TP), P(FS, None), P(FS, TP), P(FS, TP), P(FS, TP))
    out_specs = (P(FS, TP), P(FS, TP), P(FS, TP), P(FS, TP))
    return jax.shard_map(body, mesh=torus, in_specs=in_specs, out_specs=out_specs, check_vma=False)
```

```python
import jax
import jax.numpy as jnp
from jax import lax
from jax.experimental import pallas as pl
from jax.experimental.pallas import tpu as pltpu
from jax.sharding import Mesh
from jax.sharding import PartitionSpec as P

HEADS = 8
DQK = 128
RANK = 256
ZH, ZL, NY, NX, NC = 8, 2, 4, 4, 2
TP = ("x", "c")
FS = ("zh", "zl", "y")
NEAR = ("zl", "y")
GROUPS = ZL * NY
PER = RANK // GROUPS
OWN = PER // ZH
FETCHES = 2
FIRST_ROWS = 47
FIRST_ZH = (5, 4)
FIRST_RANKS = 5
FIRST_SUM = 6
FIRST_UPDATES = 6
FIRST_SQUARES = 5

F32 = jnp.float32
BF16 = jnp.bfloat16


def vmem(count):
    return [pl.BlockSpec(memory_space=pltpu.VMEM)] * count


def call(kernel, out, operands, scalars=(), scratch=(), specs=None, flops=200_000, limit=4 << 20, name=None):
    single = not isinstance(out, (list, tuple))
    moved = sum(a.size * a.dtype.itemsize for a in operands)
    return pl.pallas_call(
        kernel,
        out_shape=out,
        in_specs=[pl.BlockSpec(memory_space=pltpu.SMEM)] * len(scalars) + (specs or vmem(len(operands))),
        out_specs=vmem(1)[0] if single else vmem(len(out)),
        scratch_shapes=list(scratch),
        cost_estimate=pl.CostEstimate(flops=flops, bytes_accessed=moved, transcendentals=0),
        compiler_params=pltpu.CompilerParams(vmem_limit_bytes=limit),
        name=name,
    )(*scalars, *operands)


def exchange(parts, axes, name, first=0):
    count = parts.shape[0]
    groups = [[(first + i) % count for i in range(count)]] if first else None
    with jax.named_scope(name):
        return lax.all_to_all(parts, axes, 0, 0, axis_index_groups=groups, tiled=True)


def copies(block, count):
    return jnp.broadcast_to(block[None], (count, *block.shape))


def pick_kernel(inputs, basis, out, held, rows, sems):
    near = pltpu.make_async_copy(basis, rows, sems.at[0])
    near.start()
    fetches = []
    for i in range(FETCHES):
        part = pl.ds(i * (held.shape[0] // FETCHES), held.shape[0] // FETCHES)
        fetches.append(pltpu.make_async_copy(inputs.at[part], held.at[part], sems.at[1 + i]))
    for fetch in fetches:
        fetch.start()
    rank = lax.broadcasted_iota(jnp.int32, (RANK, PER), 0)
    slot = lax.broadcasted_iota(jnp.int32, (RANK, PER), 1)
    wanted = (slot // OWN) * PER + OWN * lax.axis_index(TP) + slot % OWN
    chosen = (rank == wanted).astype(F32).astype(BF16)
    near.wait()
    mine = jnp.dot(rows[...], chosen, preferred_element_type=F32)
    wide = jnp.concatenate([mine[8 * q : 8 * q + 8] for q in range(4)], axis=1)
    out[...] = copies(wide.astype(BF16), out.shape[0])
    for fetch in fetches:
        fetch.wait()


def project_kernel(inputs, columns, out):
    got = columns[...].astype(F32)
    if FIRST_ROWS:
        got = jnp.concatenate([got[-FIRST_ROWS:], got[:-FIRST_ROWS]], axis=0)
    lane = lax.broadcasted_iota(jnp.int32, got.shape, 2) // PER
    basis = jnp.concatenate([jnp.where(lane == q, got, 0.0) for q in range(4)], axis=1)
    basis = basis.reshape(inputs.shape[1], DQK).astype(BF16)
    low = jnp.dot(inputs[...], basis, preferred_element_type=F32).T
    low = (low[:PER] + low[PER : 2 * PER]) + (low[2 * PER : 3 * PER] + low[3 * PER :])
    high = low.astype(BF16)
    rest = (low - high.astype(F32)).astype(BF16)
    out[...] = copies(jnp.concatenate([high, rest], axis=0), out.shape[0])


def low_kernel(both, cot, out):
    low = both[...].reshape(GROUPS * 2 * PER, both.shape[2])
    low = jnp.dot(low, cot[...], preferred_element_type=F32).reshape(GROUPS, 2 * PER, DQK)
    low = low[:, :PER] + low[:, PER:]
    for g in range(GROUPS):
        out[(g - FIRST_SUM) % GROUPS] = low[(g - FIRST_RANKS) % GROUPS]


def sum_kernel(parts, first, second, out):
    out[:, :PER, :] = copies(jnp.sum(parts[...], axis=0), ZH)
    pair = jnp.concatenate([first[...], second[...]], axis=0)
    out[:, PER:, :] = copies(pair, ZH)


def moments_kernel(parts, out, first_own, second_own, fn, sn):
    low = jnp.sum(parts[:, :PER, :], axis=0)
    start = jnp.where(lax.axis_index("zl") == 0, FIRST_ZH[0], FIRST_ZH[1])
    turn = [lax.rem(z + ZH - start, ZH) for z in range(ZH)]
    first = jnp.concatenate([parts[t, PER : PER + OWN, :] for t in turn], axis=0)
    second = jnp.concatenate([parts[t, PER + OWN : PER + 2 * OWN, :] for t in turn], axis=0)
    first_new = 0.8 * first + 0.2 * low
    second_new = 0.9 * second + 0.1 * low * low
    fn[...] = first_new
    sn[...] = second_new
    out[...] = copies(first_new / jnp.sqrt(second_new), GROUPS)
    rows = pl.ds(OWN * lax.axis_index("zh"), OWN)
    first_own[...] = fn[rows, :]
    second_own[...] = sn[rows, :]


def apply_kernel(parts, basis, squares_out, step_out):
    update = jnp.concatenate(
        [
            parts[(g - FIRST_UPDATES) % GROUPS, OWN * z : OWN * (z + 1), :]
            for z in range(ZH)
            for g in range(GROUPS)
        ],
        axis=0,
    )
    squares = jnp.sum(jnp.sum(update * update, axis=0, keepdims=True), axis=1, keepdims=True)
    squares_out[...] = jnp.broadcast_to(squares[None], squares_out.shape)
    high = update.astype(BF16)
    left = update - high.astype(F32)
    mid = left.astype(BF16)
    small = (left - mid.astype(F32)).astype(BF16)
    rows = basis[...]
    step = jnp.dot(rows, small, preferred_element_type=F32)
    step += jnp.dot(rows, mid, preferred_element_type=F32)
    step_out[...] = step + jnp.dot(rows, high, preferred_element_type=F32)


def scale_kernel(squares, own, raw, master, first, second, step_out, first_out, second_out, copy_out):
    whole = jnp.sum(squares[...], axis=0) / (RANK * HEADS * DQK)
    head = own[0] / (RANK * DQK)
    step = raw[...] * (1.0 / jnp.sqrt(head + whole))
    step_out[...] = step
    copy_out[...] = (master[...] + step).astype(BF16)
    first_out[...] = first[...]
    second_out[...] = second[...]


def body(inputs, query_cot, query_basis, query_master, query_first, query_second):
    sds = jax.ShapeDtypeStruct
    tokens, small = inputs.shape[0], sds(query_first.shape, F32)
    columns, held = call(
        pick_kernel,
        (sds((ZH * GROUPS, 8, DQK), BF16), sds(inputs.shape, BF16)),
        [pltpu.with_memory_space_constraint(a, pltpu.HBM) for a in (inputs, query_basis)],
        specs=[pl.BlockSpec(memory_space=pltpu.HBM)] * 2,
        scratch=[pltpu.VMEM(query_basis.shape, BF16), pltpu.SemaphoreType.DMA((1 + FETCHES,))],
        limit=4 << 20,
        name="pick",
    )
    columns = exchange(columns, FS, "columns", FIRST_ROWS)
    both = call(
        project_kernel,
        sds((GROUPS, 2 * PER, tokens), BF16),
        (held, columns),
        flops=400_000_000,
        limit=16 << 20,
        name="project",
    )
    both = exchange(both, TP, "ranks", FIRST_RANKS)
    low = call(low_kernel, sds((GROUPS, PER, DQK), F32), (both, query_cot), name="low")
    low = exchange(low, NEAR, "near_sum", FIRST_SUM)
    low = call(
        sum_kernel,
        sds((ZH, PER + 2 * OWN, DQK), F32),
        (low, query_first, query_second),
        name="sum_near",
    )
    groups = [[(FIRST_ZH[b] + i) % ZH * ZL + b for i in range(ZH)] for b in range(ZL)]
    with jax.named_scope("far_sum"):
        low = lax.all_to_all(low, ("zh", "zl"), 0, 0, axis_index_groups=groups, tiled=True)
    update, first_new, second_new = call(
        moments_kernel,
        (sds((GROUPS, PER, DQK), F32), small, small),
        (low,),
        scratch=[pltpu.VMEM((PER, DQK), F32)] * 2,
        name="moments",
    )
    update = exchange(update, NEAR, "updates", FIRST_UPDATES)
    squares, step = call(
        apply_kernel,
        (sds((HEADS, 1, DQK), F32), sds(query_master.shape, F32)),
        (update, query_basis),
        name="apply",
    )
    heads = exchange(squares, TP, "squares", FIRST_SQUARES)
    step, first_new, second_new, copy = call(
        scale_kernel,
        (sds(query_master.shape, F32), small, small, sds(query_master.shape, BF16)),
        (heads, squares, step, query_master, first_new, second_new),
        name="scale",
    )
    return (step, first_new, second_new, copy)


def solution(mesh):
    torus = Mesh(mesh.devices.reshape(ZH, ZL, NY, NX, NC), (*FS, *TP))
    in_specs = (P(FS, None), P(FS, TP), P(FS, None), P(FS, TP), P(FS, TP), P(FS, TP))
    out_specs = (P(FS, TP), P(FS, TP), P(FS, TP), P(FS, TP))
    return jax.shard_map(body, mesh=torus, in_specs=in_specs, out_specs=out_specs, check_vma=False)
```

```python
import jax
import jax.numpy as jnp
from jax import lax
from jax.experimental import pallas as pl
from jax.experimental.pallas import tpu as pltpu
from jax.sharding import Mesh
from jax.sharding import PartitionSpec as P

HEADS = 8
DQK = 128
RANK = 256
ZH, ZL, NY, NX, NC = 8, 2, 4, 4, 2
TP = ("x", "c")
FS = ("zh", "zl", "y")
NEAR = ("zl", "y")
GROUPS = ZL * NY
PER = RANK // GROUPS
OWN = PER // ZH
FETCHES = 2
FIRST_ROWS = 47
FIRST_ZH = (5, 4)
FIRST_RANKS = 5
FIRST_SUM = 6
FIRST_UPDATES = 6
FIRST_SQUARES = 5

F32 = jnp.float32
BF16 = jnp.bfloat16


def vmem(count):
    return [pl.BlockSpec(memory_space=pltpu.VMEM)] * count


def call(kernel, out, operands, scalars=(), scratch=(), specs=None, flops=200_000, limit=4 << 20, name=None):
    single = not isinstance(out, (list, tuple))
    moved = sum(a.size * a.dtype.itemsize for a in operands)
    return pl.pallas_call(
        kernel,
        out_shape=out,
        in_specs=[pl.BlockSpec(memory_space=pltpu.SMEM)] * len(scalars) + (specs or vmem(len(operands))),
        out_specs=vmem(1)[0] if single else vmem(len(out)),
        scratch_shapes=list(scratch),
        cost_estimate=pl.CostEstimate(flops=flops, bytes_accessed=moved, transcendentals=0),
        compiler_params=pltpu.CompilerParams(vmem_limit_bytes=limit),
        name=name,
    )(*scalars, *operands)


def exchange(parts, axes, name, first=0):
    count = parts.shape[0]
    groups = [[(first + i) % count for i in range(count)]] if first else None
    with jax.named_scope(name):
        return lax.all_to_all(parts, axes, 0, 0, axis_index_groups=groups, tiled=True)


def copies(block, count):
    return jnp.broadcast_to(block[None], (count, *block.shape))


def pick_kernel(inputs, basis, out, held, rows, sems):
    near = pltpu.make_async_copy(basis, rows, sems.at[0])
    near.start()
    fetches = []
    for i in range(FETCHES):
        part = pl.ds(i * (held.shape[0] // FETCHES), held.shape[0] // FETCHES)
        fetches.append(pltpu.make_async_copy(inputs.at[part], held.at[part], sems.at[1 + i]))
    for fetch in fetches:
        fetch.start()
    rank = lax.broadcasted_iota(jnp.int32, (RANK, DQK), 0)
    slot = lax.broadcasted_iota(jnp.int32, (RANK, DQK), 1) % PER
    wanted = (slot // OWN) * PER + OWN * lax.axis_index(TP) + slot % OWN
    chosen = (rank == wanted).astype(F32).astype(BF16)
    near.wait()
    mine = jnp.dot(rows[...], chosen, preferred_element_type=F32)
    lane = lax.broadcasted_iota(jnp.int32, (8, DQK), 1) // PER
    wide = sum(jnp.where(lane == q, mine[8 * q : 8 * q + 8], 0.0) for q in range(4))
    out[...] = copies(wide.astype(BF16), out.shape[0])
    for fetch in fetches:
        fetch.wait()


def project_kernel(inputs, columns, out):
    got = columns[...].astype(F32)
    if FIRST_ROWS:
        got = jnp.concatenate([got[-FIRST_ROWS:], got[:-FIRST_ROWS]], axis=0)
    lane = lax.broadcasted_iota(jnp.int32, got.shape, 2) // PER
    basis = jnp.concatenate([jnp.where(lane == q, got, 0.0) for q in range(4)], axis=1)
    basis = basis.reshape(inputs.shape[1], DQK).astype(BF16)
    low = jnp.dot(inputs[...], basis, preferred_element_type=F32).T
    low = (low[:PER] + low[PER : 2 * PER]) + (low[2 * PER : 3 * PER] + low[3 * PER :])
    high = low.astype(BF16)
    rest = (low - high.astype(F32)).astype(BF16)
    out[...] = copies(jnp.concatenate([high, rest], axis=0), out.shape[0])


def low_kernel(both, cot, out):
    low = both[...].reshape(GROUPS * 2 * PER, both.shape[2])
    low = jnp.dot(low, cot[...], preferred_element_type=F32).reshape(GROUPS, 2 * PER, DQK)
    low = low[:, :PER] + low[:, PER:]
    for g in range(GROUPS):
        out[(g - FIRST_SUM) % GROUPS] = low[(g - FIRST_RANKS) % GROUPS]


def sum_kernel(parts, first, second, out):
    out[:, :PER, :] = copies(jnp.sum(parts[...], axis=0), ZH)
    pair = jnp.concatenate([first[...], second[...]], axis=0)
    out[:, PER:, :] = copies(pair, ZH)


def moments_kernel(parts, out, first_own, second_own, fn, sn):
    low = jnp.sum(parts[:, :PER, :], axis=0)
    start = jnp.where(lax.axis_index("zl") == 0, FIRST_ZH[0], FIRST_ZH[1])
    turn = [lax.rem(z + ZH - start, ZH) for z in range(ZH)]
    first = jnp.concatenate([parts[t, PER : PER + OWN, :] for t in turn], axis=0)
    second = jnp.concatenate([parts[t, PER + OWN : PER + 2 * OWN, :] for t in turn], axis=0)
    first_new = 0.8 * first + 0.2 * low
    second_new = 0.9 * second + 0.1 * low * low
    fn[...] = first_new
    sn[...] = second_new
    out[...] = copies(first_new / jnp.sqrt(second_new), GROUPS)
    rows = pl.ds(OWN * lax.axis_index("zh"), OWN)
    first_own[...] = fn[rows, :]
    second_own[...] = sn[rows, :]


def apply_kernel(parts, basis, squares_out, step_out):
    update = jnp.concatenate(
        [
            parts[(g - FIRST_UPDATES) % GROUPS, OWN * z : OWN * (z + 1), :]
            for z in range(ZH)
            for g in range(GROUPS)
        ],
        axis=0,
    )
    squares = jnp.sum(jnp.sum(update * update, axis=0, keepdims=True), axis=1, keepdims=True)
    squares_out[...] = jnp.broadcast_to(squares[None], squares_out.shape)
    high = update.astype(BF16)
    left = update - high.astype(F32)
    mid = left.astype(BF16)
    small = (left - mid.astype(F32)).astype(BF16)
    rows = basis[...]
    step = jnp.dot(rows, small, preferred_element_type=F32)
    step += jnp.dot(rows, mid, preferred_element_type=F32)
    step_out[...] = step + jnp.dot(rows, high, preferred_element_type=F32)


def scale_kernel(squares, own, raw, master, first, second, step_out, first_out, second_out, copy_out):
    whole = jnp.sum(squares[...], axis=0) / (RANK * HEADS * DQK)
    head = own[0] / (RANK * DQK)
    step = raw[...] * (1.0 / jnp.sqrt(head + whole))
    step_out[...] = step
    copy_out[...] = (master[...] + step).astype(BF16)
    first_out[...] = first[...]
    second_out[...] = second[...]


def body(inputs, query_cot, query_basis, query_master, query_first, query_second):
    sds = jax.ShapeDtypeStruct
    tokens, small = inputs.shape[0], sds(query_first.shape, F32)
    columns, held = call(
        pick_kernel,
        (sds((ZH * GROUPS, 8, DQK), BF16), sds(inputs.shape, BF16)),
        [pltpu.with_memory_space_constraint(a, pltpu.HBM) for a in (inputs, query_basis)],
        specs=[pl.BlockSpec(memory_space=pltpu.HBM)] * 2,
        scratch=[pltpu.VMEM(query_basis.shape, BF16), pltpu.SemaphoreType.DMA((1 + FETCHES,))],
        limit=4 << 20,
        name="pick",
    )
    columns = exchange(columns, FS, "columns", FIRST_ROWS)
    both = call(
        project_kernel,
        sds((GROUPS, 2 * PER, tokens), BF16),
        (held, columns),
        flops=400_000_000,
        limit=16 << 20,
        name="project",
    )
    both = exchange(both, TP, "ranks", FIRST_RANKS)
    low = call(low_kernel, sds((GROUPS, PER, DQK), F32), (both, query_cot), name="low")
    low = exchange(low, NEAR, "near_sum", FIRST_SUM)
    low = call(
        sum_kernel,
        sds((ZH, PER + 2 * OWN, DQK), F32),
        (low, query_first, query_second),
        name="sum_near",
    )
    groups = [[(FIRST_ZH[b] + i) % ZH * ZL + b for i in range(ZH)] for b in range(ZL)]
    with jax.named_scope("far_sum"):
        low = lax.all_to_all(low, ("zh", "zl"), 0, 0, axis_index_groups=groups, tiled=True)
    update, first_new, second_new = call(
        moments_kernel,
        (sds((GROUPS, PER, DQK), F32), small, small),
        (low,),
        scratch=[pltpu.VMEM((PER, DQK), F32)] * 2,
        name="moments",
    )
    update = exchange(update, NEAR, "updates", FIRST_UPDATES)
    squares, step = call(
        apply_kernel,
        (sds((HEADS, 1, DQK), F32), sds(query_master.shape, F32)),
        (update, query_basis),
        name="apply",
    )
    heads = exchange(squares, TP, "squares", FIRST_SQUARES)
    step, first_new, second_new, copy = call(
        scale_kernel,
        (sds(query_master.shape, F32), small, small, sds(query_master.shape, BF16)),
        (heads, squares, step, query_master, first_new, second_new),
        name="scale",
    )
    return (step, first_new, second_new, copy)


def solution(mesh):
    torus = Mesh(mesh.devices.reshape(ZH, ZL, NY, NX, NC), (*FS, *TP))
    in_specs = (P(FS, None), P(FS, TP), P(FS, None), P(FS, TP), P(FS, TP), P(FS, TP))
    out_specs = (P(FS, TP), P(FS, TP), P(FS, TP), P(FS, TP))
    return jax.shard_map(body, mesh=torus, in_specs=in_specs, out_specs=out_specs, check_vma=False)
```
